32 devices in a mesh: fs: 8 (over z, y), tp: 4 (over x, core).
Axes of the slice: x: 2, y: 2, z: 4, core: 2. Of those that a mesh axis runs over, the one named last changes fastest.
Arguments:
- tokens: bfloat16 [16, 384, 2048], P('fs', None, 'tp'), may hold values from -34 to 34
- mix_gain: float32 [2048], replicated, may hold values from 0.1 to 1.9
- w_bgate: float32 [2048, 2048], P('fs', 'tp'), may hold values from -0.125 to 0.125
- w_cgate: float32 [2048, 2048], P('fs', 'tp'), may hold values from -0.125 to 0.125
- w_value: float32 [2048, 2048], P('fs', 'tp'), may hold values from -0.125 to 0.125
- in_scale: float32 [3, 2048], P(None, 'tp'), may hold values from 0.5 to 2
- mix_taps: float32 [3, 2048], P(None, 'tp'), may hold values from -3.5 to 3.5
- w_mixout: float32 [2048, 2048], P('tp', 'fs'), may hold values from -0.125 to 0.125
- mixout_scale: float32 [1, 2048], P(None, 'fs'), may hold values from 0.5 to 2
- ffn_gain: float32 [2048], replicated, may hold values from 0.1 to 1.9
- w_upgate: float32 [2048, 5632], P('fs', 'tp'), may hold values from -0.125 to 0.125
- w_upval: float32 [2048, 5632], P('fs', 'tp'), may hold values from -0.125 to 0.125
- up_scale: float32 [2, 5632], P(None, 'tp'), may hold values from 0.5 to 2
- ffn_taps: float32 [2, 3, 5632], P(None, None, 'tp'), may hold values from -3.5 to 3.5
- w_down: float32 [5632, 2048], P('tp', 'fs'), may hold values from -0.078125 to 0.078125
- down_scale: float32 [1, 2048], P(None, 'fs'), may hold values from 0.5 to 2
Outputs:
- layer_out: bfloat16 [16, 384, 2048], P('fs', None, 'tp')
The draws below stay inside these ranges and needn't reach their ends.
All inputs are finite; a program needn't handle non-finite values.
Results may differ from the reference program's by a relative error of at most 0.015.
Values may be sent and summed in bfloat16 or wider, within the bound.
No kernel may reach another device: no remote copies, remote signals or barrier semaphores. Data moves between devices by JAX's collectives and lax.ppermute only.
A program may use at most 64 MiB of HBM per device.

```python
import math
import jax
import jax.numpy as jnp
from jax import lax

D = 2048
FF = 5632
CONV = 3
LEN = 384
SEQS = 16
N_TP = 4


def draw_tokens(key, part):
    key_base, key_rows, key_cols = jax.random.split(key, 3)
    base = jax.random.normal(key_base, (SEQS, LEN, D), jnp.float32)
    base = jnp.clip(base, -4.0, 4.0)
    row_scale = jnp.exp(jax.random.uniform(key_rows, (SEQS, LEN, 1), jnp.float32, math.log(0.3), math.log(3.0)))
    rising = jnp.exp(math.log(4.0) * (jnp.arange(D, dtype=jnp.float32) / D - 0.5))
    col_scale = rising * jax.random.uniform(key_cols, (D,), jnp.float32, 0.7, 1.4)
    return (base * row_scale * col_scale).astype(jnp.bfloat16)


def block_levels(own_key, shape, cuts, smallest, high):
    factor_of, own = 1.0, jax.random.fold_in(own_key, 6)
    for position, shards_of in cuts:
        draws = jnp.exp(jax.random.uniform(jax.random.fold_in(own, position), (shards_of,), jnp.float32, smallest / len(cuts), high / len(cuts)))
        factor_of = factor_of * jnp.repeat(draws, shape[position] // shards_of).reshape([-1 if axis == position else 1 for axis in range(len(shape))])
    return factor_of


def gaussian(rng, shape, spread, most, cuts=(), kind=jnp.bfloat16):
    loudness = block_levels(rng, shape, cuts, -0.22, 0.18) if cuts else 1.0
    drawn = jax.random.normal(rng, shape, jnp.float32) * spread * loudness
    return jnp.minimum(jnp.maximum(drawn, -most), most).astype(kind)


def setup_inputs(seed: int = 0) -> dict:
    streams_of = jax.random.split(jax.random.key(seed), 17)
    return {
        "tokens": draw_tokens(jax.random.fold_in(streams_of[16], 71), 0),
        "mix_gain": jnp.clip(1.0 + 0.18 * jax.random.normal(streams_of[1], (D,), jnp.float32), 0.1, 1.9),
        "w_bgate": gaussian(streams_of[2], (D, D), D ** -0.5, 0.125, ((0, 8), (1, 4)), jnp.float32),
        "w_cgate": gaussian(streams_of[3], (D, D), D ** -0.5, 0.125, ((0, 8), (1, 4)), jnp.float32),
        "w_value": gaussian(streams_of[4], (D, D), D ** -0.5, 0.125, ((0, 8), (1, 4)), jnp.float32),
        "in_scale": jnp.clip(jnp.exp(math.log(2.0) - 1.3862944 * jax.random.uniform(streams_of[5], (3, D), jnp.float32) ** block_levels(streams_of[5], (3, D), ((1, 4),), -0.2, 0.2)), 0.5, 2.0),
        "mix_taps": gaussian(streams_of[6], (CONV, D), CONV ** -0.5, 3.5, ((1, 4),), jnp.float32),
        "w_mixout": gaussian(streams_of[7], (D, D), D ** -0.5, 0.125, ((0, 4), (1, 8)), jnp.float32),
        "mixout_scale": jnp.clip(jnp.exp(math.log(2.0) - 1.3862944 * jax.random.uniform(streams_of[8], (1, D), jnp.float32) ** block_levels(streams_of[8], (1, D), ((1, 8),), -0.2, 0.2)), 0.5, 2.0),
        "ffn_gain": jnp.clip(1.0 + 0.18 * jax.random.normal(streams_of[9], (D,), jnp.float32), 0.1, 1.9),
        "w_upgate": gaussian(streams_of[10], (D, FF), D ** -0.5, 0.125, ((0, 8), (1, 4)), jnp.float32),
        "w_upval": gaussian(streams_of[11], (D, FF), D ** -0.5, 0.125, ((0, 8), (1, 4)), jnp.float32),
        "up_scale": jnp.clip(jnp.exp(math.log(2.0) - 1.3862944 * jax.random.uniform(streams_of[12], (2, FF), jnp.float32) ** block_levels(streams_of[12], (2, FF), ((1, 4),), -0.2, 0.2)), 0.5, 2.0),
        "ffn_taps": gaussian(streams_of[13], (2, CONV, FF), CONV ** -0.5, 3.5, ((2, 4),), jnp.float32),
        "w_down": gaussian(streams_of[14], (FF, D), FF ** -0.5, 0.078125, ((0, 4), (1, 8)), jnp.float32),
        "down_scale": jnp.clip(jnp.exp(math.log(2.0) - 1.3862944 * jax.random.uniform(streams_of[15], (1, D), jnp.float32) ** block_levels(streams_of[15], (1, D), ((1, 8),), -0.2, 0.2)), 0.5, 2.0),
    }


EPS = 1e-06

def normed_rows(values, gain):
    floats = values.astype(jnp.float32)
    factor = lax.rsqrt(lax.optimization_barrier(jnp.mean(floats * floats, axis=-1, keepdims=True)) + EPS)
    return (floats * factor * gain).astype(jnp.bfloat16).reshape(SEQS * LEN, D)

def causal_taps(values, taps):
    padded = jnp.pad(values, ((0, 0), (CONV - 1, 0), (0, 0)))
    result = jnp.zeros(values.shape, jnp.float32)
    for offset in range(CONV):
        result = result + padded[:, offset:offset + LEN] * taps[offset]
    return result

def project(inputs, matrix, scale):
    return jnp.dot(inputs, matrix.astype(jnp.bfloat16), preferred_element_type=jnp.float32) * scale

def blocked_sum(inputs, matrix, scale):
    inner_width = inputs.shape[1] // N_TP
    total = jnp.zeros((inputs.shape[0], matrix.shape[1]), jnp.float32)
    for block in range(N_TP):
        lower = block * inner_width
        part_out = jnp.dot(inputs[:, lower:lower + inner_width], matrix[lower:lower + inner_width].astype(jnp.bfloat16), preferred_element_type=jnp.float32) * scale
        rounded = lax.optimization_barrier(part_out.astype(jnp.bfloat16))
        total = total + rounded.astype(jnp.float32)
    return total

def reference(tokens, mix_gain, w_bgate, w_cgate, w_value, in_scale, mix_taps, w_mixout, mixout_scale, ffn_gain, w_upgate, w_upval, up_scale, ffn_taps, w_down, down_scale):
    row_count = SEQS * LEN
    normed = normed_rows(tokens, mix_gain)
    bgate = project(normed, w_bgate, in_scale[0])
    cgate = project(normed, w_cgate, in_scale[1])
    value = project(normed, w_value, in_scale[2])
    inner = (cgate * value).reshape(SEQS, LEN, D)
    convolved = causal_taps(inner, mix_taps)
    gated = (bgate.reshape(SEQS, LEN, D) * convolved).astype(jnp.bfloat16).reshape(row_count, D)
    mix = blocked_sum(gated, w_mixout, mixout_scale)
    resid = (tokens.reshape(row_count, D).astype(jnp.float32) + mix).astype(jnp.bfloat16)
    normed_ffn = normed_rows(resid.reshape(SEQS, LEN, D), ffn_gain)
    gate_pre = project(normed_ffn, w_upgate, up_scale[0]).reshape(SEQS, LEN, FF)
    val_pre = project(normed_ffn, w_upval, up_scale[1]).reshape(SEQS, LEN, FF)
    gate_conv = causal_taps(gate_pre, ffn_taps[0])
    val_conv = causal_taps(val_pre, ffn_taps[1])
    active = (jax.nn.silu(gate_conv) * val_conv).astype(jnp.bfloat16).reshape(row_count, FF)
    ffn = blocked_sum(active, w_down, down_scale)
    layer_out = (resid.astype(jnp.float32) + ffn).astype(jnp.bfloat16)
    return layer_out.reshape(SEQS, LEN, D)
```

```python
import jax
import jax.numpy as jnp
from jax import lax
from jax.sharding import Mesh, PartitionSpec as P

EPS = 1e-06
PLANE = ("y", "x", "c")


def split_axes(mesh):
    fs, tp = mesh.shape["fs"], mesh.shape["tp"]
    cores = 2 if tp % 2 == 0 else 1
    nx = tp // cores
    ny = nx if fs % nx == 0 else 1
    return fs // ny, ny, nx, cores


def pick(pieces, index):
    out = pieces[0]
    for i in range(1, len(pieces)):
        out = jnp.where(index == i, pieces[i], out)
    return out


def pieces_of(values, axis, count):
    size = values.shape[axis] // count
    return [lax.slice_in_dim(values, i * size, (i + 1) * size, axis=axis) for i in range(count)]


def ring(axis, shift):
    n = lax.axis_size(axis)
    return [(i, (i + shift) % n) for i in range(n)]


def exchange(pieces, axis):
    n = lax.axis_size(axis)
    own = lax.axis_index(axis)
    out = [pick(pieces, own)]
    for s in range(1, n):
        out.append(lax.ppermute(pick(pieces, (own + s) % n), axis, ring(axis, s)))
    return out


def line_gather(chunk):
    n = lax.axis_size("z")
    own = lax.axis_index("z")
    ups, downs = [chunk], [chunk]
    for s in range(1, n):
        ups.append(lax.ppermute(ups[-1], "z", [(i, i + 1) for i in range(s - 1, n - 1)]))
        downs.append(lax.ppermute(downs[-1], "z", [(i, i - 1) for i in range(1, n - s + 1)]))
    return [chunk] + [jnp.where(own >= s, ups[s], downs[n - s]) for s in range(1, n)]


def gather_weight(parts):
    nz, ny = lax.axis_size("z"), lax.axis_size("y")
    z, y = lax.axis_index("z"), lax.axis_index("y")
    shape = parts[0].shape
    out = jnp.zeros((nz, ny) + shape, parts[0].dtype)
    zero = jnp.zeros((), z.dtype)
    for t in range(ny):
        for s, chunk in enumerate(line_gather(parts[t])):
            at = ((z - s) % nz, (y - t) % ny) + (zero,) * len(shape)
            out = lax.dynamic_update_slice(out, chunk[None, None], at)
    return out


def causal_taps(values, taps):
    length = values.shape[1]
    kernel = taps.shape[0]
    padded = jnp.pad(values, ((0, 0), (kernel - 1, 0), (0, 0)))
    result = jnp.zeros(values.shape, jnp.float32)
    for offset in range(kernel):
        result = result + padded[:, offset : offset + length] * taps[offset]
    return result


def plane_rows(shard):
    wide = lax.all_gather(shard, ("x", "c"), axis=2, tiled=True)
    return lax.all_gather(wide, "y", axis=0, tiled=True)


def normed_rows(values, gain):
    floats = values.astype(jnp.float32)
    factor = lax.rsqrt(jnp.mean(floats * floats, axis=-1, keepdims=True) + EPS)
    result = (floats * factor * gain).astype(jnp.bfloat16)
    return result.reshape(-1, result.shape[-1])


def dot_rows(inputs, matrix):
    return jnp.dot(inputs, matrix, preferred_element_type=jnp.float32)


def reduce_along(values, axis, dim):
    got = exchange(pieces_of(values, dim, lax.axis_size(axis)), axis)
    total = got[0].astype(jnp.float32)
    for part in got[1:]:
        total = total + part.astype(jnp.float32)
    return total


def column_blocks(acts, blocks, scales):
    flat = blocks.reshape((-1,) + blocks.shape[2:])
    outs = [dot_rows(acts, flat[g]) for g in range(flat.shape[0])]
    return (jnp.concatenate(outs, axis=1) * scales).astype(jnp.bfloat16)


def scatter_rows(terms):
    part = terms
    part = reduce_along(part, "c", 2).astype(jnp.bfloat16)
    part = reduce_along(part, "x", 1).astype(jnp.bfloat16)
    part = part.reshape(part.shape[0], -1)
    return reduce_along(part, "y", 0)


def on_device(
    tokens,
    mix_gain,
    w_bgate,
    w_cgate,
    w_value,
    in_scale,
    mix_taps,
    w_mixout,
    mixout_scale,
    ffn_gain,
    w_upgate,
    w_upval,
    up_scale,
    ffn_taps,
    w_down,
    down_scale,
):
    ny, nx, nc = lax.axis_size("y"), lax.axis_size("x"), lax.axis_size("c")
    y = lax.axis_index("y")
    seq_count, length, own_width = tokens.shape
    row_count = seq_count * length
    seqs = seq_count * ny

    def mine(values, axis):
        return pick(pieces_of(values, axis, ny), y)

    def exchanged(matrix, axis):
        return exchange([p.astype(jnp.bfloat16) for p in pieces_of(matrix, axis, ny)], "y")

    mix_scales, down_scales = (
        lax.all_gather(mixout_scale, ("z", "y"), axis=1, tiled=True),
        lax.all_gather(down_scale, ("z", "y"), axis=1, tiled=True),
    )

    def gather_columns(*matrices):
        parts = [exchanged(m, 1) for m in matrices]
        return gather_weight([jnp.concatenate(p, axis=1) for p in zip(*parts)])

    win = gather_columns(w_bgate, w_cgate, w_value)
    wmix = gather_weight(exchanged(w_mixout, 0))
    wgate = gather_columns(w_upgate)
    wval = gather_columns(w_upval)
    wdown = gather_weight(exchanged(w_down, 0))

    normed = normed_rows(plane_rows(tokens), mix_gain)
    scales = mine(in_scale, 1)
    mixed = dot_rows(normed, win.reshape(-1, win.shape[-1]))
    bgate, cgate, value = pieces_of(mixed, 1, 3)
    bgate = bgate * scales[0]
    inner = cgate * scales[1] * (value * scales[2])
    width = inner.shape[1]
    convolved = causal_taps(inner.reshape(seqs, length, width), mine(mix_taps, 1))
    gated = (bgate.reshape(seqs, length, width) * convolved).astype(jnp.bfloat16).reshape(-1, width)
    terms = column_blocks(gated, wmix, mix_scales)
    mix = scatter_rows(terms.reshape(terms.shape[0], nx, -1))
    resid = (tokens.reshape(row_count, own_width).astype(jnp.float32) + mix).astype(jnp.bfloat16)

    normed_ffn = normed_rows(plane_rows(resid.reshape(seq_count, length, own_width)), ffn_gain)
    scales = mine(up_scale, 1)
    taps = mine(ffn_taps, 2)
    ff = wgate.shape[-1]
    gate_pre = dot_rows(normed_ffn, wgate.reshape(-1, ff)) * scales[0]
    val_pre = dot_rows(normed_ffn, wval.reshape(-1, ff)) * scales[1]
    gate_conv = causal_taps(gate_pre.reshape(seqs, length, ff), taps[0])
    val_conv = causal_taps(val_pre.reshape(seqs, length, ff), taps[1])
    active = (jax.nn.silu(gate_conv) * val_conv).astype(jnp.bfloat16).reshape(-1, ff)
    terms = column_blocks(active, wdown, down_scales)
    ffn = scatter_rows(terms.reshape(terms.shape[0], nx, -1))
    layer_out = (resid.astype(jnp.float32) + ffn).astype(jnp.bfloat16)
    return layer_out.reshape(seq_count, length, own_width)


def solution(mesh):
    fine = Mesh(mesh.devices.reshape(split_axes(mesh)), ("z",) + PLANE)
    fs, tp = ("z", "y"), ("x", "c")
    in_specs = (
        P(fs, None, tp),
        P(),
        P(fs, tp),
        P(fs, tp),
        P(fs, tp),
        P(None, tp),
        P(None, tp),
        P(tp, fs),
        P(None, fs),
        P(),
        P(fs, tp),
        P(fs, tp),
        P(None, tp),
        P(None, None, tp),
        P(tp, fs),
        P(None, fs),
    )
    out_specs = P(fs, None, tp)
    return jax.shard_map(
        on_device, mesh=fine, in_specs=in_specs, out_specs=out_specs, check_vma=False
    )
```

```python
import jax
import jax.numpy as jnp
from jax import lax
from jax.experimental import pallas as pl
from jax.experimental.pallas import tpu as pltpu
from jax.sharding import Mesh, PartitionSpec as P

EPS = 1e-06
LANES = 128
PAIR = [(0, 1), (1, 0)]
PLANE = ("y", "x", "c")


def split_axes(mesh):
    fs, tp = mesh.shape["fs"], mesh.shape["tp"]
    cores = 2 if tp % 2 == 0 else 1
    nx = tp // cores
    ny = nx if fs % nx == 0 else 1
    return fs // ny, ny, nx, cores


def pick(pieces, index):
    out = pieces[0]
    for i in range(1, len(pieces)):
        out = jnp.where(index == i, pieces[i], out)
    return out


def pieces_of(values, axis, count):
    size = values.shape[axis] // count
    return [lax.slice_in_dim(values, i * size, (i + 1) * size, axis=axis) for i in range(count)]


def ring(axis, shift):
    n = lax.axis_size(axis)
    return [(i, (i + shift) % n) for i in range(n)]


def exchange(pieces, axis):
    n = lax.axis_size(axis)
    own = lax.axis_index(axis)
    out = [pick(pieces, own)]
    for s in range(1, n):
        out.append(lax.ppermute(pick(pieces, (own + s) % n), axis, ring(axis, s)))
    return out


def line_gather(chunk):
    n = lax.axis_size("z")
    own = lax.axis_index("z")
    ups, downs = [chunk], [chunk]
    for s in range(1, n):
        ups.append(lax.ppermute(ups[-1], "z", [(i, i + 1) for i in range(s - 1, n - 1)]))
        downs.append(lax.ppermute(downs[-1], "z", [(i, i - 1) for i in range(1, n - s + 1)]))
    return [chunk] + [jnp.where(own >= s, ups[s], downs[n - s]) for s in range(1, n)]


def gather_weight(parts):
    nz, ny = lax.axis_size("z"), lax.axis_size("y")
    z, y = lax.axis_index("z"), lax.axis_index("y")
    shape = parts[0].shape
    out = jnp.zeros((nz, ny) + shape, parts[0].dtype)
    zero = jnp.zeros((), z.dtype)
    for t in range(ny):
        for s, chunk in enumerate(line_gather(parts[t])):
            at = ((z - s) % nz, (y - t) % ny) + (zero,) * len(shape)
            out = lax.dynamic_update_slice(out, chunk[None, None], at)
    return out


def causal_taps(values, taps):
    length = values.shape[1]
    kernel = taps.shape[0]
    padded = jnp.pad(values, ((0, 0), (kernel - 1, 0), (0, 0)))
    result = jnp.zeros(values.shape, jnp.float32)
    for offset in range(kernel):
        result = result + padded[:, offset : offset + length] * taps[offset]
    return result


def plane_rows(shard):
    wide = lax.all_gather(shard, ("x", "c"), axis=2, tiled=True)
    return lax.all_gather(wide, "y", axis=0, tiled=True)


def normed_rows(values, gain):
    floats = values.astype(jnp.float32)
    factor = lax.rsqrt(jnp.mean(floats * floats, axis=-1, keepdims=True) + EPS)
    result = (floats * factor * gain).astype(jnp.bfloat16)
    return result.reshape(-1, result.shape[-1])


def dot_rows(inputs, matrix):
    return jnp.dot(inputs, matrix, preferred_element_type=jnp.float32)


def reduce_along(values, axis, dim):
    got = exchange(pieces_of(values, dim, lax.axis_size(axis)), axis)
    total = got[0].astype(jnp.float32)
    for part in got[1:]:
        total = total + part.astype(jnp.float32)
    return total


def column_blocks(acts, blocks, scales):
    flat = blocks.reshape((-1,) + blocks.shape[2:])
    outs = [dot_rows(acts, flat[g]) for g in range(flat.shape[0])]
    return (jnp.concatenate(outs, axis=1) * scales).astype(jnp.bfloat16)


def scatter_rows(terms):
    part = terms
    part = reduce_along(part, "c", 2).astype(jnp.bfloat16)
    part = reduce_along(part, "x", 1).astype(jnp.bfloat16)
    part = part.reshape(part.shape[0], -1)
    return reduce_along(part, "y", 0)


def on_device_plain(
    tokens,
    mix_gain,
    w_bgate,
    w_cgate,
    w_value,
    in_scale,
    mix_taps,
    w_mixout,
    mixout_scale,
    ffn_gain,
    w_upgate,
    w_upval,
    up_scale,
    ffn_taps,
    w_down,
    down_scale,
):
    ny, nx, nc = lax.axis_size("y"), lax.axis_size("x"), lax.axis_size("c")
    y = lax.axis_index("y")
    seq_count, length, own_width = tokens.shape
    row_count = seq_count * length
    seqs = seq_count * ny

    def mine(values, axis):
        return pick(pieces_of(values, axis, ny), y)

    def exchanged(matrix, axis):
        return exchange([p.astype(jnp.bfloat16) for p in pieces_of(matrix, axis, ny)], "y")

    mix_scales, down_scales = (
        lax.all_gather(mixout_scale, ("z", "y"), axis=1, tiled=True),
        lax.all_gather(down_scale, ("z", "y"), axis=1, tiled=True),
    )

    def gather_columns(*matrices):
        parts = [exchanged(m, 1) for m in matrices]
        return gather_weight([jnp.concatenate(p, axis=1) for p in zip(*parts)])

    win = gather_columns(w_bgate, w_cgate, w_value)
    wmix = gather_weight(exchanged(w_mixout, 0))
    wgate = gather_columns(w_upgate)
    wval = gather_columns(w_upval)
    wdown = gather_weight(exchanged(w_down, 0))

    normed = normed_rows(plane_rows(tokens), mix_gain)
    scales = mine(in_scale, 1)
    mixed = dot_rows(normed, win.reshape(-1, win.shape[-1]))
    bgate, cgate, value = pieces_of(mixed, 1, 3)
    bgate = bgate * scales[0]
    inner = cgate * scales[1] * (value * scales[2])
    width = inner.shape[1]
    convolved = causal_taps(inner.reshape(seqs, length, width), mine(mix_taps, 1))
    gated = (bgate.reshape(seqs, length, width) * convolved).astype(jnp.bfloat16).reshape(-1, width)
    terms = column_blocks(gated, wmix, mix_scales)
    mix = scatter_rows(terms.reshape(terms.shape[0], nx, -1))
    resid = (tokens.reshape(row_count, own_width).astype(jnp.float32) + mix).astype(jnp.bfloat16)

    normed_ffn = normed_rows(plane_rows(resid.reshape(seq_count, length, own_width)), ffn_gain)
    scales = mine(up_scale, 1)
    taps = mine(ffn_taps, 2)
    ff = wgate.shape[-1]
    gate_pre = dot_rows(normed_ffn, wgate.reshape(-1, ff)) * scales[0]
    val_pre = dot_rows(normed_ffn, wval.reshape(-1, ff)) * scales[1]
    gate_conv = causal_taps(gate_pre.reshape(seqs, length, ff), taps[0])
    val_conv = causal_taps(val_pre.reshape(seqs, length, ff), taps[1])
    active = (jax.nn.silu(gate_conv) * val_conv).astype(jnp.bfloat16).reshape(-1, ff)
    terms = column_blocks(active, wdown, down_scales)
    ffn = scatter_rows(terms.reshape(terms.shape[0], nx, -1))
    layer_out = (resid.astype(jnp.float32) + ffn).astype(jnp.bfloat16)
    return layer_out.reshape(seq_count, length, own_width)


def split_terms(values):
    high = lax.reduce_precision(values, 8, 7)
    rest = values - high
    middle = lax.reduce_precision(rest, 8, 7)
    return [t.astype(jnp.bfloat16) for t in (high, middle, rest - middle)]


def swap(values, axis):
    return lax.ppermute(values, axis, PAIR)


def call(kernel, grid, in_specs, out_specs, out_shape, scratch, flops, order, *arrays):
    return pl.pallas_call(
        kernel,
        grid_spec=pltpu.PrefetchScalarGridSpec(
            num_scalar_prefetch=1,
            grid=grid,
            in_specs=in_specs,
            out_specs=out_specs,
            scratch_shapes=scratch,
        ),
        out_shape=out_shape,
        cost_estimate=pl.CostEstimate(flops=flops, bytes_accessed=8 << 20, transcendentals=0),
        compiler_params=pltpu.CompilerParams(
            dimension_semantics=("arbitrary",), vmem_limit_bytes=56 << 20
        ),
    )(order, *arrays)


def whole(array):
    rank = array.ndim
    return pl.BlockSpec(array.shape, lambda i, order: (0,) * rank)


def shifted_rows(values, shift):
    row = lax.broadcasted_iota(jnp.int32, values.shape, 0)
    return jnp.where(row >= shift, pltpu.roll(values, shift, axis=0), 0.0)


def conv_rows(values, taps):
    last = taps.shape[0] - 1
    total = values * taps[last : last + 1]
    for k in range(last):
        total = total + shifted_rows(values, last - k) * taps[k : k + 1]
    return total


def norm_into(order, blocks, gain, rows):
    squares = 0.0
    for block in blocks:
        floats = block[...].astype(jnp.float32)
        squares = squares + jnp.sum(floats * floats, axis=-1, keepdims=True)
    width = blocks[0].shape[-1]
    factor = lax.rsqrt(squares / (width * len(blocks)) + EPS)
    for j, block in enumerate(blocks):
        at = order[j]
        normed = block[...].astype(jnp.float32) * factor * gain[at]
        rows[:, pl.ds(pl.multiple_of(at * width, LANES), width)] = normed.astype(jnp.bfloat16)


def out_blocks(order, acts, weight, scale, keep, send):
    for j, target in enumerate((keep, send)):
        for jx in range(2):
            at = order[2 * j + jx]
            for h in range(2):
                terms = scale(at, h).astype(jnp.float32)
                total = terms[0:1] + terms[1:2] + terms[2:3]
                part = jnp.dot(acts, weight(at, h), preferred_element_type=jnp.float32)
                target[jx, h] = (part * total).astype(jnp.bfloat16)


def mixer_kernel(order, b0, b1, b2, b3, gain, weights, scales, taps, keep, send, rows):
    norm_into(order, (b0, b1, b2, b3), gain, rows)
    width = weights.shape[-1]
    unit = weights.shape[0] * weights.shape[1]
    k = rows.shape[1] // unit

    def project(m):
        matrix = weights[:, :, m * k : (m + 1) * k, :].reshape(unit * k, width)
        result = jnp.dot(rows[...], matrix, preferred_element_type=jnp.float32)
        return result * scales[m : m + 1]

    inner = project(1) * project(2)
    gated = (project(0) * conv_rows(inner, taps[...])).astype(jnp.bfloat16)
    low = 3 * k
    out_blocks(
        order,
        gated,
        lambda at, h: weights[at, h, low : low + width, :],
        lambda at, h: weights[at, h, low + width :, :],
        keep,
        send,
    )


def up_kernel(order, b0, b1, b2, b3, gain, weights, scales, taps, active, rows):
    norm_into(order, (b0, b1, b2, b3), gain, rows)
    both = weights.shape[-1]
    hidden = both // 2
    matrix = weights[...].reshape(rows.shape[1], both)
    pre = jnp.dot(rows[...], matrix, preferred_element_type=jnp.float32) * scales[...]
    conv = conv_rows(pre, taps[...])
    full = hidden // LANES * LANES
    gate, value = conv[:, :full], conv[:, both - full :]
    active[:, :full] = (gate / (1.0 + jnp.exp(-gate)) * value).astype(jnp.bfloat16)
    if full < hidden:
        mixed = conv[:, full : full + LANES]
        other = pltpu.roll(mixed, LANES // 2, axis=1)
        part = mixed / (1.0 + jnp.exp(-mixed)) * other
        active[:, full:] = part[:, : hidden - full].astype(jnp.bfloat16)


def down_kernel(order, active, weights, scales, keep, send):
    out_blocks(
        order,
        active[...],
        lambda at, h: weights[at, h],
        lambda at, h: scales[at, h],
        keep,
        send,
    )


def term_shapes(seqs, length, width):
    shape = jax.ShapeDtypeStruct((2, 2, seqs * length, width), jnp.bfloat16)
    spec = pl.BlockSpec((2, 2, length, width), lambda i, order: (0, 0, i, 0))
    return (shape, shape), (spec, spec)


def plane_blocks(own):
    half = own.shape[1] // 2
    across, beside = swap(own, "x"), swap(own, "y")
    twin = swap(own, "c")
    corner = jnp.concatenate([swap(beside[:, :half], "x"), swap(across[:, half:], "y")], axis=1)
    mine = (own, across, twin, swap(across, "c"))
    theirs = (beside, corner, swap(beside, "c"), swap(corner, "c"))
    return mine, theirs


def plane_sums(mine, theirs):
    def over_cores(terms):
        keep, send = terms
        got = swap(send, "c")
        return keep.astype(jnp.float32) + got.astype(jnp.float32)

    def moved(values, axis):
        return swap(values.astype(jnp.bfloat16), axis).astype(jnp.float32)

    far, near = over_cores(theirs), over_cores(mine)
    left_far = far[0, 0] + moved(far[1, 0], "x")
    right = near[:, 1] + moved(far[:, 1], "y")
    left_near = near[0, 0] + moved(near[1, 0], "x")
    return left_near + moved(left_far, "y"), right[0] + moved(right[1], "x")


def on_device(
    tokens,
    mix_gain,
    w_bgate,
    w_cgate,
    w_value,
    in_scale,
    mix_taps,
    w_mixout,
    mixout_scale,
    ffn_gain,
    w_upgate,
    w_upval,
    up_scale,
    ffn_taps,
    w_down,
    down_scale,
):
    y, x, c = (lax.axis_index(a) for a in PLANE)
    seqs, length, own_width = tokens.shape
    row_count = seqs * length
    blocks = 4

    def exchanged(lower, upper):
        keep, send = pick([lower, upper], y), pick([upper, lower], y)
        got = swap(send, "y")
        return jnp.stack([pick([keep, got], y), pick([got, keep], y)])

    def halves(matrix, axis):
        return pieces_of(matrix, axis, 2)

    def packed(gate, value):
        full = gate.shape[-1] // LANES * LANES
        return jnp.concatenate([gate, value[..., full:], value[..., :full]], axis=-1)

    def rounded(matrix):
        return matrix.astype(jnp.bfloat16)

    spare = jnp.zeros((10, mixout_scale.shape[1]), jnp.bfloat16)
    scale_rows = jnp.concatenate(split_terms(mixout_scale) + split_terms(down_scale) + [spare])
    ins = [halves(rounded(m), 1) for m in (w_bgate, w_cgate, w_value)]
    outs = halves(rounded(w_mixout), 0)
    mixer_half = [
        jnp.concatenate([m[i] for m in ins] + [outs[i], scale_rows]) for i in range(2)
    ]
    ups = [
        packed(g, v) for g, v in zip(halves(rounded(w_upgate), 1), halves(rounded(w_upval), 1))
    ]
    mixer_w = lax.all_gather(exchanged(*mixer_half), "z")
    up_w = lax.all_gather(exchanged(*ups), "z")
    down_w = lax.all_gather(exchanged(*halves(rounded(w_down), 0)), "z")

    order = jnp.stack(
        [jx * 2 + jc for jc in (c, 1 - c) for jx in (x, 1 - x)]
    ).astype(jnp.int32)

    def mine(values, axis):
        return pick(halves(values, axis), y)

    def block_specs(width):
        return [pl.BlockSpec((length, width), lambda i, order: (i, 0))] * blocks

    features = own_width * blocks
    rows_scratch = [pltpu.VMEM((length, features), jnp.bfloat16)]

    def mixer(group):
        small = (mix_gain.reshape(blocks, 1, own_width), mixer_w, mine(in_scale, 1), mine(mix_taps, 1))
        shapes, specs = term_shapes(seqs, length, mixer_w.shape[-1])
        flops = 2 * row_count * features * mixer_w.shape[-1] * 4
        return call(
            mixer_kernel, (seqs,), block_specs(own_width) + [whole(a) for a in small], specs, shapes,
            rows_scratch, flops, order, *group, *small,
        )

    def up(group):
        scale = packed(*(mine(up_scale, 1)[i : i + 1] for i in range(2)))
        taps = packed(*(mine(ffn_taps, 2)[i] for i in range(2)))
        small = (ffn_gain.reshape(blocks, 1, own_width), up_w, scale, taps)
        hidden = up_w.shape[-1] // 2
        flops = 2 * row_count * features * 2 * hidden
        return call(
            up_kernel, (seqs,), block_specs(own_width) + [whole(a) for a in small],
            pl.BlockSpec((length, hidden), lambda i, order: (i, 0)),
            jax.ShapeDtypeStruct((row_count, hidden), jnp.bfloat16),
            rows_scratch, flops, order, *group, *small,
        )

    down_terms = mixer_w[:, :, -13:, :]

    def down(active):
        hidden = active.shape[1]
        shapes, specs = term_shapes(seqs, length, down_w.shape[-1])
        flops = 2 * row_count * features * hidden
        return call(
            down_kernel, (seqs,),
            [pl.BlockSpec((length, hidden), lambda i, order: (i, 0)), whole(down_w), whole(down_terms)],
            specs, shapes, [], flops, order, active, down_w, down_terms,
        )

    own = tokens.reshape(row_count, own_width)
    near, far = plane_blocks(own)
    left, right = plane_sums(mixer(near), mixer(far))
    mix = jnp.concatenate([left, right], axis=1)
    resid = (own.astype(jnp.float32) + mix).astype(jnp.bfloat16)
    near, far = plane_blocks(resid)
    active_near, active_far = up(near), up(far)
    left, right = plane_sums(down(active_near), down(active_far))
    ffn = jnp.concatenate([left, right], axis=1)
    layer_out = (resid.astype(jnp.float32) + ffn).astype(jnp.bfloat16)
    return layer_out.reshape(seqs, length, own_width)


def fits(tokens, w_bgate, w_mixout, w_upgate, w_down):
    ny, nx, nc, nz = (lax.axis_size(a) for a in PLANE + ("z",))
    return (
        (ny, nx, nc) == (2, 2, 2)
        and nz * ny * w_bgate.shape[0] == nx * nc * tokens.shape[2]
        and nz == nx * nc
        and w_bgate.shape[0] == w_bgate.shape[1] // ny == w_mixout.shape[0] // ny == w_mixout.shape[1]
        and w_down.shape[1] == w_mixout.shape[1]
        and w_mixout.shape[1] % (2 * LANES) == 0
        and tokens.shape[1] % 16 == 0
        and w_upgate.shape[1] // ny % (LANES // 2) == 0
        and w_down.shape[0] // ny % 16 == 0
    )


def dispatch(*args):
    plan = on_device if fits(args[0], args[2], args[7], args[10], args[14]) else on_device_plain
    return plan(*args)


def solution(mesh):
    fine = Mesh(mesh.devices.reshape(split_axes(mesh)), ("z",) + PLANE)
    fs, tp = ("z", "y"), ("x", "c")
    in_specs = (
        P(fs, None, tp),
        P(),
        P(fs, tp),
        P(fs, tp),
        P(fs, tp),
        P(None, tp),
        P(None, tp),
        P(tp, fs),
        P(None, fs),
        P(),
        P(fs, tp),
        P(fs, tp),
        P(None, tp),
        P(None, None, tp),
        P(tp, fs),
        P(None, fs),
    )
    out_specs = P(fs, None, tp)
    return jax.shard_map(
        dispatch, mesh=fine, in_specs=in_specs, out_specs=out_specs, check_vma=False
    )
```

```python
import jax
import jax.numpy as jnp
from jax import lax
from jax.experimental import pallas as pl
from jax.experimental.pallas import tpu as pltpu
from jax.sharding import Mesh, PartitionSpec as P

EPS = 1e-06
LANES = 128
PAIR = [(0, 1), (1, 0)]
PLANE = ("y", "x", "c")


def split_axes(mesh):
    fs, tp = mesh.shape["fs"], mesh.shape["tp"]
    cores = 2 if tp % 2 == 0 else 1
    nx = tp // cores
    ny = nx if fs % nx == 0 else 1
    return fs // ny, ny, nx, cores


def pick(pieces, index):
    out = pieces[0]
    for i in range(1, len(pieces)):
        out = jnp.where(index == i, pieces[i], out)
    return out


def pieces_of(values, axis, count):
    size = values.shape[axis] // count
    return [lax.slice_in_dim(values, i * size, (i + 1) * size, axis=axis) for i in range(count)]


def ring(axis, shift):
    n = lax.axis_size(axis)
    return [(i, (i + shift) % n) for i in range(n)]


def exchange(pieces, axis):
    n = lax.axis_size(axis)
    own = lax.axis_index(axis)
    out = [pick(pieces, own)]
    for s in range(1, n):
        out.append(lax.ppermute(pick(pieces, (own + s) % n), axis, ring(axis, s)))
    return out


def line_hop(chunks, step):
    n = lax.axis_size("z")
    up, down = chunks
    return (
        lax.ppermute(up, "z", [(i, i + 1) for i in range(step - 1, n - 1)]),
        lax.ppermute(down, "z", [(i, i - 1) for i in range(1, n - step + 1)]),
    )


def line_order(hops):
    n = lax.axis_size("z")
    own = lax.axis_index("z")
    return [hops[0][0]] + [jnp.where(own >= s, hops[s][0], hops[n - s][1]) for s in range(1, n)]


def line_gather(chunk):
    hops = [(chunk, chunk)]
    for step in range(1, lax.axis_size("z")):
        hops.append(line_hop(hops[-1], step))
    return line_order(hops)


def gather_weight(parts):
    nz, ny = lax.axis_size("z"), lax.axis_size("y")
    z, y = lax.axis_index("z"), lax.axis_index("y")
    shape = parts[0].shape
    out = jnp.zeros((nz, ny) + shape, parts[0].dtype)
    zero = jnp.zeros((), z.dtype)
    for t in range(ny):
        for s, chunk in enumerate(line_gather(parts[t])):
            at = ((z - s) % nz, (y - t) % ny) + (zero,) * len(shape)
            out = lax.dynamic_update_slice(out, chunk[None, None], at)
    return out


def causal_taps(values, taps):
    length = values.shape[1]
    kernel = taps.shape[0]
    padded = jnp.pad(values, ((0, 0), (kernel - 1, 0), (0, 0)))
    result = jnp.zeros(values.shape, jnp.float32)
    for offset in range(kernel):
        result = result + padded[:, offset : offset + length] * taps[offset]
    return result


def plane_rows(shard):
    wide = lax.all_gather(shard, ("x", "c"), axis=2, tiled=True)
    return lax.all_gather(wide, "y", axis=0, tiled=True)


def normed_rows(values, gain):
    floats = values.astype(jnp.float32)
    factor = lax.rsqrt(jnp.mean(floats * floats, axis=-1, keepdims=True) + EPS)
    result = (floats * factor * gain).astype(jnp.bfloat16)
    return result.reshape(-1, result.shape[-1])


def dot_rows(inputs, matrix):
    return jnp.dot(inputs, matrix, preferred_element_type=jnp.float32)


def reduce_along(values, axis, dim):
    got = exchange(pieces_of(values, dim, lax.axis_size(axis)), axis)
    total = got[0].astype(jnp.float32)
    for part in got[1:]:
        total = total + part.astype(jnp.float32)
    return total


def column_blocks(acts, blocks, scales):
    flat = blocks.reshape((-1,) + blocks.shape[2:])
    outs = [dot_rows(acts, flat[g]) for g in range(flat.shape[0])]
    return (jnp.concatenate(outs, axis=1) * scales).astype(jnp.bfloat16)


def scatter_rows(terms):
    part = terms
    part = reduce_along(part, "c", 2).astype(jnp.bfloat16)
    part = reduce_along(part, "x", 1).astype(jnp.bfloat16)
    part = part.reshape(part.shape[0], -1)
    return reduce_along(part, "y", 0)


def on_device_plain(
    tokens,
    mix_gain,
    w_bgate,
    w_cgate,
    w_value,
    in_scale,
    mix_taps,
    w_mixout,
    mixout_scale,
    ffn_gain,
    w_upgate,
    w_upval,
    up_scale,
    ffn_taps,
    w_down,
    down_scale,
):
    ny, nx = lax.axis_size("y"), lax.axis_size("x")
    y = lax.axis_index("y")
    seq_count, length, own_width = tokens.shape
    row_count = seq_count * length
    seqs = seq_count * ny

    def mine(values, axis):
        return pick(pieces_of(values, axis, ny), y)

    def exchanged(matrix, axis):
        return exchange([p.astype(jnp.bfloat16) for p in pieces_of(matrix, axis, ny)], "y")

    mix_scales, down_scales = (
        lax.all_gather(mixout_scale, ("z", "y"), axis=1, tiled=True),
        lax.all_gather(down_scale, ("z", "y"), axis=1, tiled=True),
    )

    def gather_columns(*matrices):
        parts = [exchanged(m, 1) for m in matrices]
        return gather_weight([jnp.concatenate(p, axis=1) for p in zip(*parts)])

    win = gather_columns(w_bgate, w_cgate, w_value)
    wmix = gather_weight(exchanged(w_mixout, 0))
    wgate = gather_columns(w_upgate)
    wval = gather_columns(w_upval)
    wdown = gather_weight(exchanged(w_down, 0))

    normed = normed_rows(plane_rows(tokens), mix_gain)
    scales = mine(in_scale, 1)
    mixed = dot_rows(normed, win.reshape(-1, win.shape[-1]))
    bgate, cgate, value = pieces_of(mixed, 1, 3)
    bgate = bgate * scales[0]
    inner = cgate * scales[1] * (value * scales[2])
    width = inner.shape[1]
    convolved = causal_taps(inner.reshape(seqs, length, width), mine(mix_taps, 1))
    gated = (bgate.reshape(seqs, length, width) * convolved).astype(jnp.bfloat16).reshape(-1, width)
    terms = column_blocks(gated, wmix, mix_scales)
    mix = scatter_rows(terms.reshape(terms.shape[0], nx, -1))
    resid = (tokens.reshape(row_count, own_width).astype(jnp.float32) + mix).astype(jnp.bfloat16)

    normed_ffn = normed_rows(plane_rows(resid.reshape(seq_count, length, own_width)), ffn_gain)
    scales = mine(up_scale, 1)
    taps = mine(ffn_taps, 2)
    ff = wgate.shape[-1]
    gate_pre = dot_rows(normed_ffn, wgate.reshape(-1, ff)) * scales[0]
    val_pre = dot_rows(normed_ffn, wval.reshape(-1, ff)) * scales[1]
    gate_conv = causal_taps(gate_pre.reshape(seqs, length, ff), taps[0])
    val_conv = causal_taps(val_pre.reshape(seqs, length, ff), taps[1])
    active = (jax.nn.silu(gate_conv) * val_conv).astype(jnp.bfloat16).reshape(-1, ff)
    terms = column_blocks(active, wdown, down_scales)
    ffn = scatter_rows(terms.reshape(terms.shape[0], nx, -1))
    layer_out = (resid.astype(jnp.float32) + ffn).astype(jnp.bfloat16)
    return layer_out.reshape(seq_count, length, own_width)


def split_terms(values):
    high = lax.reduce_precision(values, 8, 7)
    rest = values - high
    middle = lax.reduce_precision(rest, 8, 7)
    return [t.astype(jnp.bfloat16) for t in (high, middle, rest - middle)]


def swap(values, axis):
    return lax.ppermute(values, axis, PAIR)


def call(kernel, grid, in_specs, out_specs, out_shape, scratch, flops, order, *arrays):
    return pl.pallas_call(
        kernel,
        grid_spec=pltpu.PrefetchScalarGridSpec(
            num_scalar_prefetch=1,
            grid=grid,
            in_specs=in_specs,
            out_specs=out_specs,
            scratch_shapes=scratch,
        ),
        out_shape=out_shape,
        cost_estimate=pl.CostEstimate(flops=flops, bytes_accessed=8 << 20, transcendentals=0),
        compiler_params=pltpu.CompilerParams(
            dimension_semantics=("arbitrary",), vmem_limit_bytes=30 << 20
        ),
    )(order, *arrays)


def whole(array):
    rank = array.ndim
    return pl.BlockSpec(array.shape, lambda i, order: (0,) * rank)


def shifted_rows(values, shift):
    row = lax.broadcasted_iota(jnp.int32, values.shape, 0)
    return jnp.where(row >= shift, pltpu.roll(values, shift, axis=0), 0.0)


def conv_rows(values, taps):
    last = taps.shape[0] - 1
    total = values * taps[last : last + 1]
    for k in range(last):
        total = total + shifted_rows(values, last - k) * taps[k : k + 1]
    return total


def norm_into(order, blocks, gain, rows):
    squares = 0.0
    for block in blocks:
        floats = block[...].astype(jnp.float32)
        squares = squares + jnp.sum(floats * floats, axis=-1, keepdims=True)
    width = blocks[0].shape[-1]
    factor = lax.rsqrt(squares / (width * len(blocks)) + EPS)
    for j, block in enumerate(blocks):
        normed = block[...].astype(jnp.float32) * factor * gain[order[j]]
        at = pl.multiple_of(order[j] * width, LANES)
        rows[:, pl.ds(at, width)] = normed.astype(jnp.bfloat16)


def scaled_terms(acts, matrix, scale):
    terms = scale.astype(jnp.float32)
    total = terms[0:1] + terms[1:2] + terms[2:3]
    part = jnp.dot(acts, matrix, preferred_element_type=jnp.float32)
    return (part * total).astype(jnp.bfloat16)


def mixer_kernel(order, b0, b1, b2, b3, gain, weights, scales, taps, keep, send, rows):
    norm_into(order, (b0, b1, b2, b3), gain, rows)
    width = weights.shape[-1]
    unit = weights.shape[0] * weights.shape[1]
    k = rows.shape[1] // unit

    def project(m):
        matrix = weights[:, :, m * k : (m + 1) * k, :].reshape(unit * k, width)
        result = jnp.dot(rows[...], matrix, preferred_element_type=jnp.float32)
        return result * scales[m : m + 1]

    inner = project(1) * project(2)
    gated = (project(0) * conv_rows(inner, taps[...])).astype(jnp.bfloat16)
    low = 3 * k
    for j in range(4):
        for h in range(2):
            matrix, scale = weights[order[j], h, low : low + width, :], weights[order[j], h, low + width :, :]
            (keep, send)[j // 2][j % 2, h] = scaled_terms(gated, matrix, scale)


def up_kernel(order, b0, b1, b2, b3, gain, weights, scales, taps, active, rows):
    norm_into(order, (b0, b1, b2, b3), gain, rows)
    both = weights.shape[-1]
    hidden = both // 2
    matrix = weights[...].reshape(rows.shape[1], both)
    pre = jnp.dot(rows[...], matrix, preferred_element_type=jnp.float32) * scales[...]
    conv = conv_rows(pre, taps[...])
    full = hidden // LANES * LANES
    gate, value = conv[:, :full], conv[:, both - full :]
    active[:, :full] = (gate / (1.0 + jnp.exp(-gate)) * value).astype(jnp.bfloat16)
    if full < hidden:
        mixed = conv[:, full : full + LANES]
        other = pltpu.roll(mixed, LANES // 2, axis=1)
        part = mixed / (1.0 + jnp.exp(-mixed)) * other
        active[:, full:] = part[:, : hidden - full].astype(jnp.bfloat16)


def down_kernel(order, active, early, late, keep, send):
    acts = active[...]
    hidden = acts.shape[1]
    for j in range(4):
        for i, weights in enumerate((late, early)):
            matrix, scale = weights[order[j], :hidden, :], weights[order[j], hidden:, :]
            (keep, send)[j // 2][j % 2, order[4 + i]] = scaled_terms(acts, matrix, scale)


def term_shapes(seqs, length, width):
    lead = (2, 2)
    shape = jax.ShapeDtypeStruct(lead + (seqs * length, width), jnp.bfloat16)
    spec = pl.BlockSpec(lead + (length, width), lambda i, order: (0, 0, i, 0))
    return (shape, shape), (spec, spec)


def plane_blocks(own):
    half = own.shape[1] // 2
    across, beside = swap(own, "x"), swap(own, "y")
    twin = swap(own, "c")
    left, right = swap(beside[:, :half], "x"), swap(across[:, half:], "y")
    corner = jnp.concatenate([left, right], axis=1)
    mine = (own, across, twin, swap(across, "c"))
    theirs = (beside, corner, swap(beside, "c"), swap(corner, "c"))
    return mine, theirs


def over_cores(terms):
    keep, send = terms
    got = swap(send, "c")
    return keep.astype(jnp.float32) + got.astype(jnp.float32)


def moved(values, axis):
    return swap(values.astype(jnp.bfloat16), axis).astype(jnp.float32)


def plane_sums(mine, theirs):
    far = over_cores(theirs)
    near = over_cores(mine)
    left_far = far[0, 0] + moved(far[1, 0], "x")
    right = near[:, 1] + moved(far[:, 1], "y")
    left_near = near[0, 0] + moved(near[1, 0], "x")
    left, right = left_near + moved(left_far, "y"), right[0] + moved(right[1], "x")
    return jnp.concatenate([left, right], axis=1)


def on_device(
    tokens,
    mix_gain,
    w_bgate,
    w_cgate,
    w_value,
    in_scale,
    mix_taps,
    w_mixout,
    mixout_scale,
    ffn_gain,
    w_upgate,
    w_upval,
    up_scale,
    ffn_taps,
    w_down,
    down_scale,
):
    y, x, c = (lax.axis_index(a) for a in PLANE)
    seqs, length, own_width = tokens.shape
    row_count = seqs * length
    blocks = 4

    def exchanged(lower, upper):
        keep, send = pick([lower, upper], y), pick([upper, lower], y)
        got = swap(send, "y")
        return jnp.stack([pick([keep, got], y), pick([got, keep], y)])

    def halves(matrix, axis):
        return pieces_of(matrix, axis, 2)

    def packed(gate, value):
        full = gate.shape[-1] // LANES * LANES
        return jnp.concatenate([gate, value[..., full:], value[..., :full]], axis=-1)

    def rounded(matrix):
        return matrix.astype(jnp.bfloat16)

    def scale_rows(scale):
        spare = jnp.zeros((13, scale.shape[1]), jnp.bfloat16)
        return jnp.concatenate(split_terms(scale) + [spare])

    z = lax.axis_index("z")
    own = tokens.reshape(row_count, own_width)

    ins = [halves(rounded(m), 1) for m in (w_bgate, w_cgate, w_value)]
    outs = halves(rounded(w_mixout), 0)
    mix_rows, down_rows = scale_rows(mixout_scale), scale_rows(down_scale)
    downs = [jnp.concatenate([d, down_rows]) for d in halves(rounded(w_down), 0)]
    early = pick(downs, y)
    hops = [(early, early)]
    hops.append(line_hop(hops[-1], 1))
    mixer_own = exchanged(*(jnp.concatenate([m[i] for m in ins] + [outs[i], mix_rows]) for i in range(2)))
    mixer_own, hops = lax.optimization_barrier((mixer_own, hops))
    mixer_w = lax.all_gather(mixer_own, "z")
    hops.append(line_hop(hops[-1], 2))
    hops.append(line_hop(hops[-1], 3))
    early_w = jnp.stack(line_order(hops))
    ups = [
        packed(g, v) for g, v in zip(halves(rounded(w_upgate), 1), halves(rounded(w_upval), 1))
    ]
    up_own = exchanged(*ups)
    up_w = lax.all_gather(up_own, "z")
    late = swap(pick(downs[::-1], y), "y")
    late_hops = [(late, late)]
    for step in (1, 2, 3):
        late_hops.append(line_hop(late_hops[-1], step))
    late_w = jnp.stack(line_order(late_hops))

    places = [jx * 2 + jc for jc in (c, 1 - c) for jx in (x, 1 - x)]

    def table(*entries):
        return jnp.stack(entries).astype(jnp.int32)

    order = table(*places)
    down_order = table(*((z - t) % blocks for t in places), 1 - y, y)

    def mine(values, axis):
        return pick(halves(values, axis), y)

    def block_specs(width):
        return [pl.BlockSpec((length, width), lambda i, order: (i, 0))] * blocks

    features = own_width * blocks
    rows_scratch = [pltpu.VMEM((length, features), jnp.bfloat16)]

    def mixer(group):
        width = mixer_w.shape[-1]
        small = (mix_gain.reshape(blocks, 1, own_width), mixer_w, mine(in_scale, 1), mine(mix_taps, 1))
        shapes, specs = term_shapes(seqs, length, width)
        flops = 2 * row_count * features * width * 4
        return call(
            mixer_kernel, (seqs,), block_specs(own_width) + [whole(a) for a in small], specs, shapes,
            rows_scratch, flops, order, *group, *small,
        )

    def up(group):
        scale = packed(*(mine(up_scale, 1)[i : i + 1] for i in range(2)))
        taps = packed(*(mine(ffn_taps, 2)[i] for i in range(2)))
        small = (ffn_gain.reshape(blocks, 1, own_width), up_w, scale, taps)
        hidden = up_w.shape[-1] // 2
        flops = 2 * row_count * features * 2 * hidden
        return call(
            up_kernel, (seqs,), block_specs(own_width) + [whole(a) for a in small],
            pl.BlockSpec((length, hidden), lambda i, order: (i, 0)),
            jax.ShapeDtypeStruct((row_count, hidden), jnp.bfloat16),
            rows_scratch, flops, order, *group, *small,
        )

    def down(active):
        hidden = active.shape[1]
        shapes, specs = term_shapes(seqs, length, early_w.shape[-1])
        flops = 2 * row_count * features * hidden
        return call(
            down_kernel, (seqs,),
            [pl.BlockSpec((length, hidden), lambda i, order: (i, 0)), whole(early_w), whole(late_w)],
            specs, shapes, [], flops, down_order, active, early_w, late_w,
        )

    def added(base, sums):
        return (base.astype(jnp.float32) + sums).astype(jnp.bfloat16)

    near, far = plane_blocks(own)
    terms_far = mixer(far)
    resid = added(own, plane_sums(mixer(near), terms_far))
    near, far = plane_blocks(resid)
    active_near, active_far = up(near), up(far)
    terms_far = down(active_far)
    layer_out = added(resid, plane_sums(down(active_near), terms_far))
    return layer_out.reshape(seqs, length, own_width)


def fits(tokens, w_bgate, w_mixout, w_upgate, w_down):
    ny, nx, nc, nz = (lax.axis_size(a) for a in PLANE + ("z",))
    return (
        (ny, nx, nc) == (2, 2, 2)
        and nz * ny * w_bgate.shape[0] == nx * nc * tokens.shape[2]
        and nz == nx * nc == 4
        and w_bgate.shape[0] == w_bgate.shape[1] // ny == w_mixout.shape[0] // ny == w_mixout.shape[1]
        and w_down.shape[1] == w_mixout.shape[1]
        and w_mixout.shape[1] % (2 * LANES) == 0
        and tokens.shape[1] % 16 == 0
        and w_upgate.shape[1] // ny % (LANES // 2) == 0
        and w_down.shape[0] // ny % 16 == 0
    )


def dispatch(*args):
    if not fits(args[0], args[2], args[7], args[10], args[14]):
        return on_device_plain(*args)
    return on_device(*args)


def solution(mesh):
    fine = Mesh(mesh.devices.reshape(split_axes(mesh)), ("z",) + PLANE)
    fs, tp = ("z", "y"), ("x", "c")
    in_specs = (
        P(fs, None, tp),
        P(),
        P(fs, tp),
        P(fs, tp),
        P(fs, tp),
        P(None, tp),
        P(None, tp),
        P(tp, fs),
        P(None, fs),
        P(),
        P(fs, tp),
        P(fs, tp),
        P(None, tp),
        P(None, None, tp),
        P(tp, fs),
        P(None, fs),
    )
    out_specs = P(fs, None, tp)
    return jax.shard_map(
        dispatch, mesh=fine, in_specs=in_specs, out_specs=out_specs, check_vma=False
    )
```

```python
import jax
import jax.numpy as jnp
from jax import lax
from jax.experimental import pallas as pl
from jax.experimental.pallas import tpu as pltpu
from jax.sharding import Mesh, PartitionSpec as P

EPS = 1e-06
LANES = 128
PAIR = [(0, 1), (1, 0)]
PLANE = ("y", "x", "c")


def split_axes(mesh):
    fs, tp = mesh.shape["fs"], mesh.shape["tp"]
    cores = 2 if tp % 2 == 0 else 1
    nx = tp // cores
    ny = nx if fs % nx == 0 else 1
    return fs // ny, ny, nx, cores


def pick(pieces, index):
    out = pieces[0]
    for i in range(1, len(pieces)):
        out = jnp.where(index == i, pieces[i], out)
    return out


def pieces_of(values, axis, count):
    size = values.shape[axis] // count
    return [lax.slice_in_dim(values, i * size, (i + 1) * size, axis=axis) for i in range(count)]


def ring(axis, shift):
    n = lax.axis_size(axis)
    return [(i, (i + shift) % n) for i in range(n)]


def exchange(pieces, axis):
    n = lax.axis_size(axis)
    own = lax.axis_index(axis)
    out = [pick(pieces, own)]
    for s in range(1, n):
        out.append(lax.ppermute(pick(pieces, (own + s) % n), axis, ring(axis, s)))
    return out


def line_gather(chunk):
    n = lax.axis_size("z")
    own = lax.axis_index("z")
    ups, downs = [chunk], [chunk]
    for s in range(1, n):
        ups.append(lax.ppermute(ups[-1], "z", [(i, i + 1) for i in range(s - 1, n - 1)]))
        downs.append(lax.ppermute(downs[-1], "z", [(i, i - 1) for i in range(1, n - s + 1)]))
    return [chunk] + [jnp.where(own >= s, ups[s], downs[n - s]) for s in range(1, n)]


def gather_weight(parts):
    nz, ny = lax.axis_size("z"), lax.axis_size("y")
    z, y = lax.axis_index("z"), lax.axis_index("y")
    shape = parts[0].shape
    out = jnp.zeros((nz, ny) + shape, parts[0].dtype)
    zero = jnp.zeros((), z.dtype)
    for t in range(ny):
        for s, chunk in enumerate(line_gather(parts[t])):
            at = ((z - s) % nz, (y - t) % ny) + (zero,) * len(shape)
            out = lax.dynamic_update_slice(out, chunk[None, None], at)
    return out


def causal_taps(values, taps):
    length = values.shape[1]
    kernel = taps.shape[0]
    padded = jnp.pad(values, ((0, 0), (kernel - 1, 0), (0, 0)))
    result = jnp.zeros(values.shape, jnp.float32)
    for offset in range(kernel):
        result = result + padded[:, offset : offset + length] * taps[offset]
    return result


def plane_rows(shard):
    wide = lax.all_gather(shard, ("x", "c"), axis=2, tiled=True)
    return lax.all_gather(wide, "y", axis=0, tiled=True)


def normed_rows(values, gain):
    floats = values.astype(jnp.float32)
    factor = lax.rsqrt(jnp.mean(floats * floats, axis=-1, keepdims=True) + EPS)
    result = (floats * factor * gain).astype(jnp.bfloat16)
    return result.reshape(-1, result.shape[-1])


def dot_rows(inputs, matrix):
    return jnp.dot(inputs, matrix, preferred_element_type=jnp.float32)


def reduce_along(values, axis, dim):
    got = exchange(pieces_of(values, dim, lax.axis_size(axis)), axis)
    total = got[0].astype(jnp.float32)
    for part in got[1:]:
        total = total + part.astype(jnp.float32)
    return total


def column_blocks(acts, blocks, scales):
    flat = blocks.reshape((-1,) + blocks.shape[2:])
    outs = [dot_rows(acts, flat[g]) for g in range(flat.shape[0])]
    return (jnp.concatenate(outs, axis=1) * scales).astype(jnp.bfloat16)


def scatter_rows(terms):
    part = terms
    part = reduce_along(part, "c", 2).astype(jnp.bfloat16)
    part = reduce_along(part, "x", 1).astype(jnp.bfloat16)
    part = part.reshape(part.shape[0], -1)
    return reduce_along(part, "y", 0)


def on_device_plain(
    tokens,
    mix_gain,
    w_bgate,
    w_cgate,
    w_value,
    in_scale,
    mix_taps,
    w_mixout,
    mixout_scale,
    ffn_gain,
    w_upgate,
    w_upval,
    up_scale,
    ffn_taps,
    w_down,
    down_scale,
):
    ny, nx = lax.axis_size("y"), lax.axis_size("x")
    y = lax.axis_index("y")
    seq_count, length, own_width = tokens.shape
    row_count = seq_count * length
    seqs = seq_count * ny

    def mine(values, axis):
        return pick(pieces_of(values, axis, ny), y)

    def exchanged(matrix, axis):
        return exchange([p.astype(jnp.bfloat16) for p in pieces_of(matrix, axis, ny)], "y")

    mix_scales, down_scales = (
        lax.all_gather(mixout_scale, ("z", "y"), axis=1, tiled=True),
        lax.all_gather(down_scale, ("z", "y"), axis=1, tiled=True),
    )

    def gather_columns(*matrices):
        parts = [exchanged(m, 1) for m in matrices]
        return gather_weight([jnp.concatenate(p, axis=1) for p in zip(*parts)])

    win = gather_columns(w_bgate, w_cgate, w_value)
    wmix = gather_weight(exchanged(w_mixout, 0))
    wgate = gather_columns(w_upgate)
    wval = gather_columns(w_upval)
    wdown = gather_weight(exchanged(w_down, 0))

    normed = normed_rows(plane_rows(tokens), mix_gain)
    scales = mine(in_scale, 1)
    mixed = dot_rows(normed, win.reshape(-1, win.shape[-1]))
    bgate, cgate, value = pieces_of(mixed, 1, 3)
    bgate = bgate * scales[0]
    inner = cgate * scales[1] * (value * scales[2])
    width = inner.shape[1]
    convolved = causal_taps(inner.reshape(seqs, length, width), mine(mix_taps, 1))
    gated = (bgate.reshape(seqs, length, width) * convolved).astype(jnp.bfloat16).reshape(-1, width)
    terms = column_blocks(gated, wmix, mix_scales)
    mix = scatter_rows(terms.reshape(terms.shape[0], nx, -1))
    resid = (tokens.reshape(row_count, own_width).astype(jnp.float32) + mix).astype(jnp.bfloat16)

    normed_ffn = normed_rows(plane_rows(resid.reshape(seq_count, length, own_width)), ffn_gain)
    scales = mine(up_scale, 1)
    taps = mine(ffn_taps, 2)
    ff = wgate.shape[-1]
    gate_pre = dot_rows(normed_ffn, wgate.reshape(-1, ff)) * scales[0]
    val_pre = dot_rows(normed_ffn, wval.reshape(-1, ff)) * scales[1]
    gate_conv = causal_taps(gate_pre.reshape(seqs, length, ff), taps[0])
    val_conv = causal_taps(val_pre.reshape(seqs, length, ff), taps[1])
    active = (jax.nn.silu(gate_conv) * val_conv).astype(jnp.bfloat16).reshape(-1, ff)
    terms = column_blocks(active, wdown, down_scales)
    ffn = scatter_rows(terms.reshape(terms.shape[0], nx, -1))
    layer_out = (resid.astype(jnp.float32) + ffn).astype(jnp.bfloat16)
    return layer_out.reshape(seq_count, length, own_width)


def split_terms(values):
    high = lax.reduce_precision(values, 8, 7)
    rest = values - high
    middle = lax.reduce_precision(rest, 8, 7)
    return [t.astype(jnp.bfloat16) for t in (high, middle, rest - middle)]


def swap(values, axis):
    return lax.ppermute(values, axis, PAIR)


def call(kernel, grid, in_specs, out_specs, out_shape, scratch, flops, order, *arrays):
    return pl.pallas_call(
        kernel,
        grid_spec=pltpu.PrefetchScalarGridSpec(
            num_scalar_prefetch=1,
            grid=grid,
            in_specs=in_specs,
            out_specs=out_specs,
            scratch_shapes=scratch,
        ),
        out_shape=out_shape,
        cost_estimate=pl.CostEstimate(flops=flops, bytes_accessed=8 << 20, transcendentals=0),
        compiler_params=pltpu.CompilerParams(
            dimension_semantics=("arbitrary",), vmem_limit_bytes=(16 if kernel is down_kernel else 28) << 20
        ),
    )(order, *arrays)


def whole(array):
    rank = array.ndim
    return pl.BlockSpec(array.shape, lambda i, order: (0,) * rank)


def shifted_rows(values, shift):
    row = lax.broadcasted_iota(jnp.int32, values.shape, 0)
    return jnp.where(row >= shift, pltpu.roll(values, shift, axis=0), 0.0)


def conv_rows(values, taps):
    last = taps.shape[0] - 1
    total = values * taps[last : last + 1]
    for k in range(last):
        total = total + shifted_rows(values, last - k) * taps[k : k + 1]
    return total


def norm_into(order, blocks, gain, rows, place):
    squares = 0.0
    for block in blocks:
        floats = block[...].astype(jnp.float32)
        squares = squares + jnp.sum(floats * floats, axis=-1, keepdims=True)
    width = blocks[0].shape[-1]
    half = width // 2
    factor = lax.rsqrt(squares / (width * len(blocks)) + EPS)
    for j, block in enumerate(blocks):
        normed = (block[...].astype(jnp.float32) * factor * gain[order[j]]).astype(jnp.bfloat16)
        for h in range(2):
            at = pl.multiple_of(place(j, h) * half, LANES)
            rows[:, pl.ds(at, half)] = normed[:, h * half : (h + 1) * half]


def scaled_terms(acts, matrix, scale):
    terms = scale.astype(jnp.float32)
    total = terms[0:1] + terms[1:2] + terms[2:3]
    part = jnp.dot(acts, matrix, preferred_element_type=jnp.float32)
    return (part * total).astype(jnp.bfloat16)


def mixer_kernel(order, b0, b1, b2, b3, gain, *refs):
    *slabs, scales, taps, keep, send, rows, last = refs
    width = slabs[0].shape[-1]
    k = rows.shape[1] // len(slabs)
    low = 3 * k
    y = order[8]

    @pl.when(pl.program_id(0) == 0)
    def _():
        for q, slab in enumerate(slabs):
            last[q] = slab[low:, :]

    norm_into(order, (b0, b1, b2, b3), gain, rows, lambda j, h: 2 * order[4 + j] + (h + y) % 2)

    def project(m):
        result = 0.0
        for q, slab in enumerate(slabs):
            acts = rows[:, q * k : (q + 1) * k]
            matrix = slab[m * k : (m + 1) * k, :]
            result = result + jnp.dot(acts, matrix, preferred_element_type=jnp.float32)
        return result * scales[m : m + 1]

    inner = project(1) * project(2)
    gated = (project(0) * conv_rows(inner, taps[...])).astype(jnp.bfloat16)
    for j in range(4):
        for h in range(2):
            at = 2 * order[4 + j] + (h + y) % 2
            terms = scaled_terms(gated, last[at, :width, :], last[at, width:, :])
            (keep, send)[j // 2][j % 2, h] = terms


def up_kernel(order, b0, b1, b2, b3, gain, weights, scales, taps, active, rows):
    norm_into(order, (b0, b1, b2, b3), gain, rows, lambda j, h: 2 * order[j] + h)
    both = weights.shape[-1]
    hidden = both // 2
    matrix = weights[...].reshape(rows.shape[1], both)
    pre = jnp.dot(rows[...], matrix, preferred_element_type=jnp.float32) * scales[...]
    conv = conv_rows(pre, taps[...])
    full = hidden // LANES * LANES
    gate, value = conv[:, :full], conv[:, both - full :]
    active[:, :full] = (gate / (1.0 + jnp.exp(-gate)) * value).astype(jnp.bfloat16)
    if full < hidden:
        mixed = conv[:, full : full + LANES]
        other = pltpu.roll(mixed, LANES // 2, axis=1)
        part = mixed / (1.0 + jnp.exp(-mixed)) * other
        active[:, full:] = part[:, : hidden - full].astype(jnp.bfloat16)


def down_kernel(order, active, weights, keep, send):
    acts = active[...]
    hidden = acts.shape[1]
    for j in range(4):
        for h in range(2):
            matrix, scale = weights[order[j], h, :hidden, :], weights[order[j], h, hidden:, :]
            (keep, send)[j // 2][j % 2, h] = scaled_terms(acts, matrix, scale)


def term_shapes(seqs, length, width):
    lead = (2, 2)
    shape = jax.ShapeDtypeStruct(lead + (seqs * length, width), jnp.bfloat16)
    spec = pl.BlockSpec(lead + (length, width), lambda i, order: (0, 0, i, 0))
    return (shape, shape), (spec, spec)


def plane_blocks(own, both=True):
    half = own.shape[1] // 2
    across = swap(own, "x")
    beside = swap(own, "y")
    twin = swap(own, "c")
    if both:
        corner = jnp.concatenate([swap(beside[:, :half], "x"), swap(across[:, half:], "y")], axis=1)
    else:
        corner = swap(beside, "x")
    mine = (own, across, twin, swap(across, "c"))
    theirs = (beside, corner, swap(beside, "c"), swap(corner, "c"))
    return mine, theirs


def over_cores(terms):
    keep, send = terms
    got = swap(send, "c")
    return keep.astype(jnp.float32) + got.astype(jnp.float32)


def moved(values, axis):
    return swap(values.astype(jnp.bfloat16), axis).astype(jnp.float32)


def plane_sums(mine, theirs):
    far = over_cores(theirs)
    near = over_cores(mine)
    left_far = far[0, 0] + moved(far[1, 0], "x")
    right = near[:, 1] + moved(far[:, 1], "y")
    left_near = near[0, 0] + moved(near[1, 0], "x")
    left = left_near + moved(left_far, "y")
    right = right[0] + moved(right[1], "x")
    return jnp.concatenate([left, right], axis=1)


def on_device(
    tokens,
    mix_gain,
    w_bgate,
    w_cgate,
    w_value,
    in_scale,
    mix_taps,
    w_mixout,
    mixout_scale,
    ffn_gain,
    w_upgate,
    w_upval,
    up_scale,
    ffn_taps,
    w_down,
    down_scale,
):
    y, x, c = (lax.axis_index(a) for a in PLANE)
    seqs, length, own_width = tokens.shape
    row_count = seqs * length
    blocks = 4

    def exchanged(lower, upper):
        keep, send = pick([lower, upper], y), pick([upper, lower], y)
        got = swap(send, "y")
        return jnp.stack([pick([keep, got], y), pick([got, keep], y)])

    def halves(matrix, axis):
        return pieces_of(matrix, axis, 2)

    def packed(gate, value):
        full = gate.shape[-1] // LANES * LANES
        return jnp.concatenate([gate, value[..., full:], value[..., :full]], axis=-1)

    def rounded(matrix):
        return matrix.astype(jnp.bfloat16)

    def scale_rows(scale):
        spare = jnp.zeros((13, scale.shape[1]), jnp.bfloat16)
        return jnp.concatenate(split_terms(scale) + [spare])

    z = lax.axis_index("z")
    inside = (z == 1) | (z == 2)
    own = tokens.reshape(row_count, own_width)
    outer = lax.ppermute(own, "z", [(0, 1), (3, 2)])

    ins = [halves(rounded(m), 1) for m in (w_bgate, w_cgate, w_value)]
    outs = halves(rounded(w_mixout), 0)
    mix_rows, down_rows = scale_rows(mixout_scale), scale_rows(down_scale)
    mixer_halves = [jnp.concatenate([m[i] for m in ins] + [outs[i], mix_rows]) for i in range(2)]
    mixer_keep = pick(mixer_halves, y)
    mixer_got = swap(pick(mixer_halves[::-1], y), "y")

    def to_inside(chunk):
        below = lax.ppermute(chunk, "z", [(0, 1), (1, 2)])
        above = lax.ppermute(chunk, "z", [(3, 2), (2, 1)])
        from_first = lax.ppermute(below, "z", [(1, 2)])
        from_last = lax.ppermute(above, "z", [(2, 1)])
        return chunk, below, above, jnp.where(z == 1, from_last, from_first)

    kept, gotten = to_inside(mixer_keep), to_inside(mixer_got)
    slabs = tuple(s for pair in zip(kept, gotten) for s in pair)
    origins = [(z + d) % blocks for d in (0, -1, 1, 2)]

    ups = [
        packed(g, v) for g, v in zip(halves(rounded(w_upgate), 1), halves(rounded(w_upval), 1))
    ]
    up_own = exchanged(*ups)
    near, far = plane_blocks(own, False)
    outer_near, outer_far = plane_blocks(outer, False)
    up_own, slabs = lax.optimization_barrier((up_own, slabs))
    up_w = lax.all_gather(up_own, "z")
    places = [jx * 2 + jc for jc in (c, 1 - c) for jx in (x, 1 - x)]

    def index_of(value, entries):
        return sum(jnp.where(value == e, i, 0) for i, e in enumerate(entries))

    def table(*entries):
        return jnp.stack(entries).astype(jnp.int32)

    mixer_order = table(*places, *(index_of(t, origins) for t in places), y)
    up_order = table(*places, *places)

    def mine(values, axis):
        return pick(halves(values, axis), y)

    def block_specs(width):
        return [pl.BlockSpec((length, width), lambda i, order: (i, 0))] * blocks

    features = own_width * blocks
    rows_scratch = [pltpu.VMEM((length, features), jnp.bfloat16)]

    def mixer(group):
        width = mixer_keep.shape[-1]
        small = (mix_gain.reshape(blocks, 1, own_width), *slabs, mine(in_scale, 1), mine(mix_taps, 1))
        shapes, specs = term_shapes(seqs, length, width)
        flops = 2 * row_count * features * width * 4
        rest = mixer_keep.shape[0] - 3 * w_mixout.shape[1]
        scratch = rows_scratch + [pltpu.VMEM((2 * blocks, rest, width), jnp.bfloat16)]
        return call(
            mixer_kernel, (seqs,), block_specs(own_width) + [whole(a) for a in small], specs, shapes,
            scratch, flops, mixer_order, *group, *small,
        )

    def up(group):
        scale = packed(*(mine(up_scale, 1)[i : i + 1] for i in range(2)))
        taps = packed(*(mine(ffn_taps, 2)[i] for i in range(2)))
        small = (ffn_gain.reshape(blocks, 1, own_width), up_w, scale, taps)
        hidden = up_w.shape[-1] // 2
        flops = 2 * row_count * features * 2 * hidden
        return call(
            up_kernel, (seqs,), block_specs(own_width) + [whole(a) for a in small],
            pl.BlockSpec((length, hidden), lambda i, order: (i, 0)),
            jax.ShapeDtypeStruct((row_count, hidden), jnp.bfloat16),
            rows_scratch, flops, up_order, *group, *small,
        )

    def down(active):
        hidden = active.shape[1]
        shapes, specs = term_shapes(seqs, length, down_w.shape[-1])
        flops = 2 * row_count * features * hidden
        return call(
            down_kernel, (seqs,),
            [pl.BlockSpec((length, hidden), lambda i, order: (i, 0)), whole(down_w)],
            specs, shapes, [], flops, up_order, active, down_w,
        )

    def added(base, sums):
        return (base.astype(jnp.float32) + sums).astype(jnp.bfloat16)

    terms_far = mixer(outer_far)
    outer_near, terms_far = lax.optimization_barrier((outer_near, terms_far))
    terms_near = mixer(outer_near)
    near, far, terms_near = lax.optimization_barrier((near, far, terms_near))
    outer_out = added(outer, plane_sums(terms_near, terms_far))
    back = lax.ppermute(outer_out, "z", [(1, 0), (2, 3)])
    terms_far = mixer(far)
    near, terms_far, w_down, down_rows = lax.optimization_barrier((near, terms_far, w_down, down_rows))
    downs = [jnp.concatenate([d, down_rows]) for d in halves(rounded(w_down), 0)]
    down_own = exchanged(*downs)
    down_w = lax.all_gather(down_own, "z")
    resid = added(own, plane_sums(mixer(near), terms_far))
    resid = jnp.where(inside, resid, back)
    near, far = plane_blocks(resid)
    active_near = up(near)
    active_far = up(far)
    terms_far = down(active_far)
    layer_out = added(resid, plane_sums(down(active_near), terms_far))
    return layer_out.reshape(seqs, length, own_width)


def fits(tokens, w_bgate, w_mixout, w_upgate, w_down):
    ny, nx, nc, nz = (lax.axis_size(a) for a in PLANE + ("z",))
    return (
        (ny, nx, nc) == (2, 2, 2)
        and nz * ny * w_bgate.shape[0] == nx * nc * tokens.shape[2]
        and nz == nx * nc == 4
        and w_bgate.shape[0] == w_bgate.shape[1] // ny == w_mixout.shape[0] // ny == w_mixout.shape[1]
        and w_down.shape[1] == w_mixout.shape[1]
        and w_mixout.shape[1] % (2 * LANES) == 0
        and tokens.shape[1] % 16 == 0
        and w_upgate.shape[1] // ny % (LANES // 2) == 0
        and w_down.shape[0] // ny % 16 == 0
    )


def dispatch(*args):
    if not fits(args[0], args[2], args[7], args[10], args[14]):
        return on_device_plain(*args)
    return on_device(*args)


def solution(mesh):
    fine = Mesh(mesh.devices.reshape(split_axes(mesh)), ("z",) + PLANE)
    fs, tp = ("z", "y"), ("x", "c")
    in_specs = (
        P(fs, None, tp),
        P(),
        P(fs, tp),
        P(fs, tp),
        P(fs, tp),
        P(None, tp),
        P(None, tp),
        P(tp, fs),
        P(None, fs),
        P(),
        P(fs, tp),
        P(fs, tp),
        P(None, tp),
        P(None, None, tp),
        P(tp, fs),
        P(None, fs),
    )
    out_specs = P(fs, None, tp)
    return jax.shard_map(
        dispatch, mesh=fine, in_specs=in_specs, out_specs=out_specs, check_vma=False
    )
```
